32 devices in a mesh: sp: 16 (over z, y, x), tp: 2 (over core).
Axes of the slice: x: 2, y: 2, z: 4, core: 2. Of those that a mesh axis runs over, the one named last changes fastest.
Arguments:
- queries: bfloat16 [24576, 1024], P('sp', 'tp'), may hold values from -6 to 6
- forget_logit: bfloat16 [24576, 1024], P('sp', 'tp'), may hold values from -8 to 8
- value_rows: bfloat16 [24576, 1024], P('sp', 'tp'), may hold values from -10 to 10
- out_gate: bfloat16 [24576, 1024], P('sp', 'tp'), may hold values from -6 to 6
- floor_gap: float32 [1024], P('tp'), may hold values from 0 to 0.1, as said below
- head_gain: float32 [1024], P('tp'), may hold values from 0.1 to 1.9
- state_in: float32 [8, 128, 128], P('tp'), may hold values from -0.625 to 0.625
- out_weight: bfloat16 [1024, 2048], P('tp'), may hold values from -0.1875 to 0.1875
Outputs:
- projected: bfloat16 [24576, 2048], P(('sp', 'tp'))
- state_out: float32 [8, 16384], P('tp', 'sp')
The draws below stay inside these ranges and needn't reach their ends.
Inputs may be any that keep to these rules, and one draw needn't show every extreme that they name: `floor_gap`: strictly between 0 and 0.1.
All inputs are finite; a program needn't handle non-finite values.
Results may differ from the reference program's by a relative error of at most 0.009.
Values may be sent and summed in bfloat16 or wider, within the bound.
A program may use at most 128 MiB of HBM per device.

```python
import jax
import jax.numpy as jnp
from jax import lax

D = 2048
HEADS = 8
KEY_DIM = 128
VAL_DIM = 128
BLOCK = 128
SPAN = 1536
LENGTH = 24576
KEY_WIDTH = 1024
VAL_WIDTH = 1024


def stretch_offsets(key, width, scale):
    segment = max(SPAN // 2, 1)
    count = LENGTH // segment
    offsets = scale * jax.random.normal(key, (count, 1, width), jnp.float32)
    return jnp.broadcast_to(offsets, (count, segment, width)).reshape(LENGTH, width)


def draw_forget_logit(key, part):
    noise_key, shift_key = jax.random.split(jax.random.fold_in(key, 11))
    noise = jnp.clip(jax.random.normal(noise_key, (LENGTH, KEY_WIDTH), jnp.float32), -4.0, 4.0)
    shift = jnp.clip(stretch_offsets(shift_key, KEY_WIDTH, 1.5), -4.0, 4.0)
    return (noise + shift).astype(jnp.bfloat16)


def draw_value_rows(key, part):
    noise_key, shift_key = jax.random.split(jax.random.fold_in(key, 13))
    noise = jnp.clip(jax.random.normal(noise_key, (LENGTH, VAL_WIDTH), jnp.float32), -4.0, 4.0)
    shift = jnp.clip(stretch_offsets(shift_key, VAL_WIDTH, 2.0), -6.0, 6.0)
    return (noise + shift).astype(jnp.bfloat16)


def draw_floor_gap(key, part):
    ranking_key, slow_key, fast_key = jax.random.split(jax.random.fold_in(key, 5), 3)
    ranking = jax.random.permutation(ranking_key, HEADS)
    fast_count = HEADS // 2
    fast_head = jnp.repeat(ranking < fast_count, KEY_DIM)
    slow_gap = jnp.exp(jax.random.uniform(slow_key, (KEY_WIDTH,), jnp.float32, jnp.log(0.5), jnp.log(2.0))) / LENGTH
    fast_gap = jnp.exp(jax.random.uniform(fast_key, (KEY_WIDTH,), jnp.float32, jnp.log(0.03), jnp.log(0.08)))
    return jnp.where(fast_head, fast_gap, slow_gap)


def levels(rng, dims, cuts, smallest, top_value):
    factor_of, own = 1.0, jax.random.fold_in(rng, 6)
    for axis_at, blocks in cuts:
        draws = jnp.exp(jax.random.uniform(jax.random.fold_in(own, axis_at), (blocks,), jnp.float32, smallest / len(cuts), top_value / len(cuts)))
        factor_of = factor_of * jnp.repeat(draws, dims[axis_at] // blocks).reshape([-1 if axis == axis_at else 1 for axis in range(len(dims))])
    return factor_of


def normal_values(key, dims, scale, most, cuts=(), dtype=jnp.bfloat16):
    level = levels(key, dims, cuts, -0.22, 0.18) if cuts else 1.0
    entries = jax.random.normal(key, dims, jnp.float32) * scale * level
    return jnp.minimum(jnp.maximum(entries, -most), most).astype(dtype)


def setup_inputs(seed: int = 0) -> dict:
    splits = jax.random.split(jax.random.key(seed), 9)
    return {
        "queries": normal_values(splits[0], (LENGTH, KEY_WIDTH), 1.0, 6.0, ((0, 16), (1, 2))),
        "forget_logit": draw_forget_logit(jax.random.fold_in(splits[8], 71), 0),
        "value_rows": draw_value_rows(jax.random.fold_in(splits[8], 71), 0),
        "out_gate": normal_values(splits[3], (LENGTH, VAL_WIDTH), 1.0, 6.0, ((0, 16), (1, 2))),
        "floor_gap": draw_floor_gap(jax.random.fold_in(splits[8], 71), 0),
        "head_gain": jnp.clip(1.0 + 0.18 * jax.random.normal(splits[5], (VAL_WIDTH,), jnp.float32), 0.1, 1.9),
        "state_in": normal_values(splits[6], (HEADS, KEY_DIM, VAL_DIM), 0.1, 0.625, ((0, 2),), jnp.float32),
        "out_weight": normal_values(splits[7], (VAL_WIDTH, D), VAL_WIDTH ** -0.5, 0.1875, ((0, 2),)),
    }


maximum_precision = lax.Precision.HIGHEST
epsilon = 1e-06

def reference(queries, forget_logit, value_rows, out_gate, floor_gap, head_gain, state_in, out_weight):
    blocks = LENGTH // BLOCK
    gap_rows = floor_gap.reshape(HEADS, KEY_DIM)
    gain_rows = head_gain.reshape(HEADS, VAL_DIM)
    causal = jnp.arange(BLOCK)[:, None] >= jnp.arange(BLOCK)[None, :]

    def to_heads(values, width):
        return values.reshape(blocks, BLOCK, HEADS, width).transpose(0, 2, 1, 3)
    inputs = (to_heads(queries, KEY_DIM), to_heads(forget_logit, KEY_DIM), to_heads(value_rows, VAL_DIM), to_heads(out_gate, VAL_DIM))

    def advance(passed_forward, pieces):
        query_block, logit_block, value_block, gate_block = pieces
        key_gate = gap_rows[:, None, :] * jax.nn.sigmoid(-logit_block.astype(jnp.float32))
        log_forget = jnp.log1p(-key_gate)
        reader = jax.nn.silu(query_block.astype(jnp.float32))
        written_update = value_block.astype(jnp.float32)
        cumul = jnp.cumsum(log_forget, axis=1)
        scaled_readout = reader * jnp.exp(cumul)
        scores = jnp.einsum('hck,hsk->hcs', scaled_readout, key_gate * jnp.exp(-cumul), precision=maximum_precision)
        scores = jnp.where(causal[None], scores, 0.0)
        unscaled_output = jnp.einsum('hcs,hsv->hcv', scores, written_update, precision=maximum_precision)
        unscaled_output = unscaled_output + jnp.einsum('ufx,uxa->ufa', scaled_readout, passed_forward, precision=maximum_precision)
        block_log_decay = cumul[:, -1]
        decay_to_finish = key_gate * jnp.exp(block_log_decay[:, None, :] - cumul)
        refreshed_state = jnp.exp(block_log_decay)[..., None] * passed_forward + jnp.einsum('lxr,lxf->lrf', decay_to_finish, written_update, precision=maximum_precision)
        mean_square = lax.optimization_barrier(jnp.mean(unscaled_output * unscaled_output, axis=-1, keepdims=True))
        normed = unscaled_output * lax.rsqrt(mean_square + epsilon) * gain_rows[:, None, :]
        gated = (normed * jax.nn.silu(gate_block.astype(jnp.float32))).astype(jnp.bfloat16)
        return (refreshed_state, gated)
    state_out, gated = lax.scan(advance, state_in, inputs)
    gated = gated.transpose(0, 2, 1, 3).reshape(LENGTH, VAL_WIDTH)
    projected = jnp.dot(gated, out_weight, preferred_element_type=jnp.float32).astype(jnp.bfloat16)
    return (projected, state_out.reshape(HEADS, KEY_DIM * VAL_DIM))
```

```python
import functools

import jax
import jax.numpy as jnp
from jax import lax
from jax.experimental import pallas as pl
from jax.experimental.pallas import tpu as pltpu
from jax.sharding import PartitionSpec as P

BLOCK = 128
TILE = 256
epsilon = 1e-06
MESH = pl.DeviceIdType.MESH
f32 = jnp.float32
bf16 = jnp.bfloat16


def nt(a, b):
    return lax.dot_general(a, b, (((1,), (1,)), ((), ())), preferred_element_type=f32)


def tn(a, b):
    return lax.dot_general(a, b, (((0,), (0,)), ((), ())), preferred_element_type=f32)


def nn(a, b):
    return jnp.dot(a, b, preferred_element_type=f32)


def kernel(
    dims,
    fl_any, v_any, q_any, og_any, gap_any, gain_any, st_any, w_any,
    out_any, so_any,
    fl, v, q, og, gap, gain, stin, wown, wpeer,
    ecum, kst, sbef, run, lt, es, raw, sg, qs2,
    sbuf, dmine, rbuf, dbuf, dall, tcol, obuf, ibuf, gsend, gown, gpeer, ob, so,
    in_sem, s1, r1, sd, rd, s2, r2, gs, gr, wsem, osem, so_sem,
):
    n, heads, blocks, kp, tiles = dims
    me = lax.axis_index("sp")
    core = lax.axis_index("tp")
    mate = 1 - core
    half = blocks // 2

    def local(i, src, dst):
        return pltpu.make_async_copy(src, dst, in_sem.at[i])

    loads = [
        local(0, fl_any, fl), local(1, v_any, v), local(2, gap_any, gap),
        local(3, q_any, q), local(4, og_any, og), local(5, gain_any, gain),
        local(6, st_any.at[:, pl.ds(me * kp, kp), :], stin), local(7, w_any, wown),
    ]
    for load in loads:
        load.start()

    barrier = pltpu.get_barrier_semaphore()

    def greet(d, c):
        pl.semaphore_signal(barrier, inc=1, device_id={"sp": lax.rem(me + d, n)}, device_id_type=MESH)
        return c

    lax.fori_loop(1, n, greet, 0)
    pl.semaphore_signal(barrier, inc=1, device_id={"tp": mate}, device_id_type=MESH)

    row = lax.broadcasted_iota(jnp.int32, (BLOCK, BLOCK), 0)
    col = lax.broadcasted_iota(jnp.int32, (BLOCK, BLOCK), 1)
    causal = row >= col
    lower = jnp.where(causal, 1.0, 0.0).astype(bf16)
    lower2 = jnp.concatenate([lower, lower], axis=1)

    run[...] = jnp.zeros_like(run)
    lt[...] = jnp.zeros_like(lt)
    dall[...] = jnp.zeros_like(dall)
    loads[0].wait()
    loads[1].wait()
    loads[2].wait()

    def first(b, c):
        rows = pl.ds(pl.multiple_of(b * BLOCK, BLOCK), BLOCK)
        es[b] = jnp.exp(lt[...])
        for h in range(heads):
            cols = slice(h * 128, (h + 1) * 128)
            x = fl[rows, cols].astype(f32)
            g = gap[:, cols] * (1.0 / (1.0 + jnp.exp(x)))
            lf = jnp.log1p(-g)
            hi = lf.astype(bf16)
            lo = (lf - hi.astype(f32)).astype(bf16)
            cum = nn(lower2, jnp.concatenate([hi, lo], axis=0))
            e = jnp.exp(cum)
            ks = g * jnp.exp(-cum)
            et = e[BLOCK - 1 : BLOCK, :]
            ecum[rows, cols] = e
            kst[rows, cols] = ks.astype(bf16)
            old = run[h]
            sbef[b, h] = old.astype(bf16)
            run[h] = old * et + tn(v[rows, cols], (ks * et).astype(bf16))
            lt[:, cols] = lt[:, cols] + cum[BLOCK - 1 : BLOCK, :]
        return c

    lax.fori_loop(0, blocks, first, 0)

    for h in range(heads):
        cols = slice(h * 128, (h + 1) * 128)
        sbuf[:, h] = run[h].T.reshape(n, kp, 128).astype(bf16)
        dmine[h : h + 1, :] = jnp.exp(lt[:, cols])

    pl.semaphore_wait(barrier, n)

    def state_copy(d):
        to = lax.rem(me + d, n)
        return pltpu.make_async_remote_copy(
            src_ref=sbuf.at[to], dst_ref=rbuf.at[me], send_sem=s1.at[d], recv_sem=r1.at[d],
            device_id={"sp": to}, device_id_type=MESH)

    def decay_copy(d):
        return pltpu.make_async_remote_copy(
            src_ref=dmine, dst_ref=dbuf.at[me], send_sem=sd.at[d], recv_sem=rd.at[d],
            device_id={"sp": lax.rem(me + d, n)}, device_id_type=MESH)

    def back_copy(d):
        to = lax.rem(me + d, n)
        return pltpu.make_async_remote_copy(
            src_ref=obuf.at[to], dst_ref=ibuf.at[me], send_sem=s2.at[d], recv_sem=r2.at[d],
            device_id={"sp": to}, device_id_type=MESH)

    def send_states(d, c):
        state_copy(d).start()
        decay_copy(d).start()
        return c

    lax.fori_loop(1, n, send_states, 0)
    weights = pltpu.make_async_remote_copy(
        src_ref=w_any, dst_ref=wpeer, send_sem=wsem.at[0], recv_sem=wsem.at[1],
        device_id={"tp": mate}, device_id_type=MESH)
    weights.start()
    rbuf[me] = sbuf[me]
    dbuf[me] = dmine[...]

    loads[3].wait()
    loads[4].wait()
    loads[5].wait()
    loads[6].wait()

    def second(b, c):
        rows = pl.ds(pl.multiple_of(b * BLOCK, BLOCK), BLOCK)
        start = es[b]
        for h in range(heads):
            cols = slice(h * 128, (h + 1) * 128)
            qv = q[rows, cols].astype(f32)
            scaled = qv * (1.0 / (1.0 + jnp.exp(-qv))) * ecum[rows, cols]
            qs = scaled.astype(bf16)
            qs2[rows, cols] = (scaled * start[:, cols]).astype(bf16)
            scores = jnp.where(causal, nt(qs, kst[rows, cols]), 0.0).astype(bf16)
            raw[rows, cols] = nn(scores, v[rows, cols]) + nt(qs, sbef[b, h])
            gv = og[rows, cols].astype(f32)
            sg[rows, cols] = gv * (1.0 / (1.0 + jnp.exp(-gv))) * gain[:, cols]
        return c

    lax.fori_loop(0, half, second, 0)

    def got_states(d, c):
        state_copy(d).wait_recv()
        decay_copy(d).wait_recv()
        return c

    lax.fori_loop(1, n, got_states, 0)

    def spread(j, c):
        dall[pl.ds(j * 8, heads), :] = dbuf[j]
        return c

    lax.fori_loop(0, n, spread, 0)
    tcol[...] = dall[...].T
    decays = tcol[pl.ds(me * kp, kp), :]
    for h in range(heads):
        state = stin[h]
        for j in range(n):
            obuf[j, h] = state.astype(bf16)
            state = decays[:, 8 * j + h : 8 * j + h + 1] * state + rbuf[j, h].astype(f32)
        for k in range(kp):
            so[h : h + 1, k * 128 : (k + 1) * 128] = state[k : k + 1, :]
    ibuf[me] = obuf[me]

    def send_back(d, c):
        back_copy(d).start()
        return c

    lax.fori_loop(1, n, send_back, 0)
    state_done = pltpu.make_async_copy(so, so_any, so_sem)
    state_done.start()

    lax.fori_loop(half, blocks, second, 0)

    def got_back(d, c):
        back_copy(d).wait_recv()
        return c

    lax.fori_loop(1, n, got_back, 0)
    incoming = [ibuf[:, h].astype(f32).reshape(n * kp, 128).astype(bf16) for h in range(heads)]

    def finish(rows, h):
        cols = slice(h * 128, (h + 1) * 128)
        out = raw[rows, cols] + nn(qs2[rows, cols], incoming[h])
        mean = jnp.mean(out * out, axis=-1, keepdims=True)
        return (out * lax.rsqrt(mean + epsilon) * sg[rows, cols]).astype(bf16)

    def gated_copy(i):
        rows = pl.ds(pl.multiple_of(i * BLOCK, BLOCK), BLOCK)
        return pltpu.make_async_remote_copy(
            src_ref=gsend.at[rows], dst_ref=gpeer.at[rows], send_sem=gs.at[i], recv_sem=gr.at[i],
            device_id={"tp": mate}, device_id_type=MESH)

    def theirs(i, c):
        rows = pl.ds(pl.multiple_of((mate * half + i) * BLOCK, BLOCK), BLOCK)
        to = pl.ds(pl.multiple_of(i * BLOCK, BLOCK), BLOCK)
        for h in range(heads):
            gsend[to, h * 128 : (h + 1) * 128] = finish(rows, h)

        @pl.when(i > 0)
        def _():
            gated_copy(i - 1).start()

        return c

    lax.fori_loop(0, half, theirs, 0)
    gated_copy(half - 1).start()

    def mine(i, c):
        rows = pl.ds(pl.multiple_of((core * half + i) * BLOCK, BLOCK), BLOCK)
        to = pl.ds(pl.multiple_of(i * BLOCK, BLOCK), BLOCK)
        for h in range(heads):
            gown[to, h * 128 : (h + 1) * 128] = finish(rows, h)
        return c

    lax.fori_loop(0, half, mine, 0)

    loads[7].wait()
    weights.wait()

    def got_gated(i, c):
        gated_copy(i).wait()
        return c

    lax.fori_loop(0, half, got_gated, 0)

    def out_copy(t):
        cols = pl.ds(pl.multiple_of(t * TILE, TILE), TILE)
        return pltpu.make_async_copy(ob.at[:, cols], out_any.at[:, cols], osem.at[t])

    def project(t, c):
        cols = pl.ds(pl.multiple_of(t * TILE, TILE), TILE)
        ob[:, cols] = (nn(gown[...], wown[:, cols]) + nn(gpeer[...], wpeer[:, cols])).astype(bf16)

        @pl.when(t > 0)
        def _():
            out_copy(t - 1).start()

        return c

    lax.fori_loop(0, tiles, project, 0)
    out_copy(tiles - 1).start()

    def sent(d, c):
        state_copy(d).wait_send()
        decay_copy(d).wait_send()
        back_copy(d).wait_send()
        return c

    lax.fori_loop(1, n, sent, 0)
    state_done.wait()

    def written(t, c):
        out_copy(t).wait()
        return c

    lax.fori_loop(0, tiles, written, 0)


def per_device(
    queries, forget_logit, value_rows, out_gate, floor_gap, head_gain, state_in, out_weight
):
    n = lax.axis_size("sp")
    rows, width = queries.shape
    heads = state_in.shape[0]
    depth = out_weight.shape[1]
    blocks = rows // BLOCK
    kp = 128 // n
    tiles = depth // TILE
    mine = rows // 2
    V = pltpu.VMEM
    D = pltpu.SemaphoreType.DMA
    scratch = [
        V((rows, width), bf16), V((rows, width), bf16), V((rows, width), bf16), V((rows, width), bf16),
        V((1, width), f32), V((1, width), f32), V((heads, kp, 128), f32),
        V((width, depth), bf16), V((width, depth), bf16),
        V((rows, width), f32), V((rows, width), bf16), V((blocks, heads, 128, 128), bf16),
        V((heads, 128, 128), f32), V((1, width), f32), V((blocks, 1, width), f32),
        V((rows, width), f32), V((rows, width), f32), V((rows, width), bf16),
        V((n, heads, kp, 128), bf16), V((heads, 128), f32), V((n, heads, kp, 128), bf16),
        V((n, heads, 128), f32), V((n * 8, 128), f32), V((128, n * 8), f32),
        V((n, heads, kp, 128), bf16), V((n, heads, kp, 128), bf16),
        V((mine, width), bf16), V((mine, width), bf16), V((mine, width), bf16),
        V((mine, depth), bf16), V((heads, kp * 128), f32),
        D((8,)), D((n,)), D((n,)), D((n,)), D((n,)), D((n,)), D((n,)),
        D((blocks // 2,)), D((blocks // 2,)), D((2,)), D((tiles,)), D(()),
    ]
    projected, state_out = pl.pallas_call(
        functools.partial(kernel, (n, heads, blocks, kp, tiles)),
        name="layer",
        out_shape=(
            jax.ShapeDtypeStruct((mine, depth), bf16),
            jax.ShapeDtypeStruct((heads, kp * 128), f32),
        ),
        in_specs=[pl.BlockSpec(memory_space=pl.ANY)] * 8,
        out_specs=(pl.BlockSpec(memory_space=pl.ANY),) * 2,
        scratch_shapes=scratch,
        compiler_params=pltpu.CompilerParams(
            collective_id=0, has_side_effects=True, vmem_limit_bytes=60 * 1024 * 1024
        ),
    )(
        forget_logit, value_rows, queries, out_gate,
        floor_gap.reshape(1, width), head_gain.reshape(1, width), state_in, out_weight,
    )
    return (projected, state_out)


def solution(mesh):
    placed = (
        P("sp", "tp"),
        P("sp", "tp"),
        P("sp", "tp"),
        P("sp", "tp"),
        P("tp"),
        P("tp"),
        P("tp", None, None),
        P("tp", None),
    )
    return jax.shard_map(
        per_device,
        mesh=mesh,
        in_specs=placed,
        out_specs=(P(("sp", "tp"), None), P("tp", "sp")),
        check_vma=False,
    )
```

```python
import functools

import jax
import jax.numpy as jnp
from jax import lax
from jax.experimental import pallas as pl
from jax.experimental.pallas import tpu as pltpu
from jax.sharding import PartitionSpec as P

BLOCK = 128
TILE = 512
epsilon = 1e-06
MESH = pl.DeviceIdType.MESH
f32 = jnp.float32
bf16 = jnp.bfloat16
VMEM_LAYER = 60 * 1024 * 1024
LOG_TERMS = (0.248358778, 0.245560933, 0.33349572, 0.49999794, 1.0)


def nt(a, b):
    return lax.dot_general(a, b, (((1,), (1,)), ((), ())), preferred_element_type=f32)


def tn(a, b):
    return lax.dot_general(a, b, (((0,), (0,)), ((), ())), preferred_element_type=f32)


def nn(a, b):
    return jnp.dot(a, b, preferred_element_type=f32)


def log_keep(g):
    series = LOG_TERMS[0]
    for term in LOG_TERMS[1:]:
        series = series * g + term
    return -g * series


def kernel(
    dims,
    fl_any, v_any, q_any, og_any, gap_any, gain_any, st_any, w_any,
    gown_out, gpeer, wpeer, so_out,
    fl, v, q, og, gap, gain, stin,
    cumul, kg, sbef, run, lt, es, raw, sg, qs2,
    hl, kst, dec, eb, qsc, gown, so,
    sbuf, dmine, rbuf, dbuf, dall, tcol, obuf, ibuf, gsend,
    in_sem, fl_sem, v_sem, s1, r1, sd, rd, s2, r2, gs, gr, wsem, gown_sem, so_sem,
):
    n, heads, blocks, kp = dims
    me = lax.axis_index("sp")
    core = lax.axis_index("tp")
    mate = 1 - core
    half = blocks // 2

    def local(i, src, dst):
        return pltpu.make_async_copy(src, dst, in_sem.at[i])

    def early(b):
        rows = pl.ds(pl.multiple_of(b * BLOCK, BLOCK), BLOCK)
        return (
            pltpu.make_async_copy(fl_any.at[rows], fl.at[rows], fl_sem.at[b]),
            pltpu.make_async_copy(v_any.at[rows], v.at[rows], v_sem.at[b]),
        )

    def start_early(b, c):
        for copy in early(b):
            copy.start()
        return c

    gap_load = local(0, gap_any, gap)
    gap_load.start()
    lax.fori_loop(0, blocks, start_early, 0)
    loads = [
        local(1, q_any, q), local(2, og_any, og), local(3, gain_any, gain),
        local(4, st_any.at[:, pl.ds(me * kp, kp), :], stin),
    ]

    barrier = pltpu.get_barrier_semaphore()

    def greet(d, c):
        pl.semaphore_signal(barrier, inc=1, device_id={"sp": lax.rem(me + d, n)}, device_id_type=MESH)
        return c

    lax.fori_loop(1, n, greet, 0)
    pl.semaphore_signal(barrier, inc=1, device_id={"tp": mate}, device_id_type=MESH)

    row = lax.broadcasted_iota(jnp.int32, (BLOCK, BLOCK), 0)
    col = lax.broadcasted_iota(jnp.int32, (BLOCK, BLOCK), 1)
    causal = row >= col
    lower = jnp.where(causal, 1.0, 0.0).astype(bf16)
    lower2 = jnp.concatenate([lower, lower], axis=1)

    run[...] = jnp.zeros_like(run)
    lt[...] = jnp.zeros_like(lt)
    dall[...] = jnp.zeros_like(dall)
    gap_load.wait()

    def block_rows(b):
        return pl.ds(pl.multiple_of(b * BLOCK, BLOCK), BLOCK)

    def gates(b, c):
        rows = block_rows(b)
        for copy in early(b):
            copy.wait()
        for h in range(heads):
            cols = slice(h * 128, (h + 1) * 128)
            x = fl[rows, cols].astype(f32)
            g = gap[:, cols] * (1.0 / (1.0 + jnp.exp(x)))
            lf = log_keep(g)
            hi = lf.astype(bf16)
            kg[rows, cols] = g
            hl[b, 0:BLOCK, cols] = hi
            hl[b, BLOCK:, cols] = (lf - hi.astype(f32)).astype(bf16)
        return c

    def sums(b, c):
        cumul[block_rows(b), :] = nn(lower2, hl[b])
        return c

    def decayed(b, c):
        rows = block_rows(b)
        es[b] = jnp.exp(lt[...])
        last = cumul[pl.ds(b * BLOCK + BLOCK - 1, 1), :]
        lt[...] = lt[...] + last
        keep = jnp.exp(last)
        eb[b] = keep
        for h in range(heads):
            cols = slice(h * 128, (h + 1) * 128)
            keys = kg[rows, cols] * jnp.exp(-cumul[rows, cols])
            kst[rows, cols] = keys.astype(bf16)
            dec[rows, cols] = (keys * keep[:, cols]).astype(bf16)
        return c

    def states(b, c):
        rows = block_rows(b)
        for h in range(heads):
            cols = slice(h * 128, (h + 1) * 128)
            old = run[h]
            sbef[b, h] = old.astype(bf16)
            run[h] = old * eb[b][:, cols] + tn(v[rows, cols], dec[rows, cols])
        return c

    with jax.named_scope("gates"):
        lax.fori_loop(0, blocks, gates, 0)
    with jax.named_scope("sums"):
        lax.fori_loop(0, blocks, sums, 0, unroll=2)
    with jax.named_scope("decayed"):
        lax.fori_loop(0, blocks, decayed, 0)
    with jax.named_scope("states"):
        lax.fori_loop(0, blocks, states, 0, unroll=2)
    for load in loads:
        load.start()

    for h in range(heads):
        cols = slice(h * 128, (h + 1) * 128)
        sbuf[:, h] = run[h].T.reshape(n, kp, 128).astype(bf16)
        dmine[h : h + 1, :] = jnp.exp(lt[:, cols])

    pl.semaphore_wait(barrier, n)

    def state_copy(d):
        to = lax.rem(me + d, n)
        return pltpu.make_async_remote_copy(
            src_ref=sbuf.at[to], dst_ref=rbuf.at[me], send_sem=s1.at[d], recv_sem=r1.at[d],
            device_id={"sp": to}, device_id_type=MESH)

    def decay_copy(d):
        return pltpu.make_async_remote_copy(
            src_ref=dmine, dst_ref=dbuf.at[me], send_sem=sd.at[d], recv_sem=rd.at[d],
            device_id={"sp": lax.rem(me + d, n)}, device_id_type=MESH)

    def back_copy(d):
        to = lax.rem(me + d, n)
        return pltpu.make_async_remote_copy(
            src_ref=obuf.at[to], dst_ref=ibuf.at[me], send_sem=s2.at[d], recv_sem=r2.at[d],
            device_id={"sp": to}, device_id_type=MESH)

    def send_states(d, c):
        state_copy(d).start()
        decay_copy(d).start()
        return c

    lax.fori_loop(1, n, send_states, 0)
    weights = pltpu.make_async_remote_copy(
        src_ref=w_any, dst_ref=wpeer, send_sem=wsem.at[0], recv_sem=wsem.at[1],
        device_id={"tp": mate}, device_id_type=MESH)
    weights.start()
    rbuf[me] = sbuf[me]
    dbuf[me] = dmine[...]

    for load in loads:
        load.wait()

    def reads(b, c):
        rows = block_rows(b)
        start = es[b]
        for h in range(heads):
            cols = slice(h * 128, (h + 1) * 128)
            hq = 0.5 * q[rows, cols].astype(f32)
            scaled = (hq + hq * jnp.tanh(hq)) * jnp.exp(cumul[rows, cols])
            qsc[rows, cols] = scaled.astype(bf16)
            qs2[rows, cols] = (scaled * start[:, cols]).astype(bf16)
            hg = 0.5 * og[rows, cols].astype(f32)
            sg[rows, cols] = (hg + hg * jnp.tanh(hg)) * gain[:, cols]
        return c

    def within(b, c):
        rows = block_rows(b)
        for h in range(heads):
            cols = slice(h * 128, (h + 1) * 128)
            qs = qsc[rows, cols]
            scores = jnp.where(causal, nt(qs, kst[rows, cols]), 0.0).astype(bf16)
            raw[rows, cols] = nn(scores, v[rows, cols]) + nt(qs, sbef[b, h])
        return c

    with jax.named_scope("reads"):
        lax.fori_loop(0, blocks, reads, 0)

    def got_states(d, c):
        state_copy(d).wait_recv()
        decay_copy(d).wait_recv()
        return c

    with jax.named_scope("wait1"):
        lax.fori_loop(1, n, got_states, 0)

    def spread(j, c):
        dall[pl.ds(j * 8, heads), :] = dbuf[j]
        return c

    lax.fori_loop(0, n, spread, 0)
    tcol[...] = dall[...].T
    decays = tcol[pl.ds(me * kp, kp), :]
    for h in range(heads):
        state = stin[h]
        for j in range(n):
            obuf[j, h] = state.astype(bf16)
            state = decays[:, 8 * j + h : 8 * j + h + 1] * state + rbuf[j, h].astype(f32)
        for k in range(kp):
            so[h : h + 1, k * 128 : (k + 1) * 128] = state[k : k + 1, :]
    ibuf[me] = obuf[me]

    def send_back(d, c):
        back_copy(d).start()
        return c

    lax.fori_loop(1, n, send_back, 0)
    state_done = pltpu.make_async_copy(so, so_out, so_sem)
    state_done.start()

    with jax.named_scope("within"):
        lax.fori_loop(0, blocks, within, 0, unroll=3)

    def got_back(d, c):
        back_copy(d).wait_recv()
        return c

    with jax.named_scope("wait2"):
        lax.fori_loop(1, n, got_back, 0)
    incoming = [ibuf[:, h].astype(f32).reshape(n * kp, 128).astype(bf16) for h in range(heads)]

    def finish(rows, h):
        cols = slice(h * 128, (h + 1) * 128)
        out = raw[rows, cols] + nn(qs2[rows, cols], incoming[h])
        mean = jnp.mean(out * out, axis=-1, keepdims=True)
        return (out * lax.rsqrt(mean + epsilon) * sg[rows, cols]).astype(bf16)

    def gated_copy(i):
        rows = pl.ds(pl.multiple_of(i * BLOCK, BLOCK), BLOCK)
        return pltpu.make_async_remote_copy(
            src_ref=gsend.at[rows], dst_ref=gpeer.at[rows], send_sem=gs.at[i], recv_sem=gr.at[i],
            device_id={"tp": mate}, device_id_type=MESH)

    def theirs(i, c):
        rows = pl.ds(pl.multiple_of((mate * half + i) * BLOCK, BLOCK), BLOCK)
        to = pl.ds(pl.multiple_of(i * BLOCK, BLOCK), BLOCK)
        for h in range(heads):
            gsend[to, h * 128 : (h + 1) * 128] = finish(rows, h)

        @pl.when(i > 0)
        def _():
            gated_copy(i - 1).start()

        return c

    with jax.named_scope("theirs"):
        lax.fori_loop(0, half, theirs, 0, unroll=2)
    gated_copy(half - 1).start()

    def mine(i, c):
        rows = pl.ds(pl.multiple_of((core * half + i) * BLOCK, BLOCK), BLOCK)
        to = pl.ds(pl.multiple_of(i * BLOCK, BLOCK), BLOCK)
        for h in range(heads):
            gown[to, h * 128 : (h + 1) * 128] = finish(rows, h)

        @pl.when(i > 0)
        def _():
            own_copy(i - 1).start()

        return c

    def own_copy(i):
        rows = block_rows(i)
        return pltpu.make_async_copy(gown.at[rows], gown_out.at[rows], gown_sem.at[i])

    with jax.named_scope("mine"):
        lax.fori_loop(0, half, mine, 0, unroll=2)
    own_copy(half - 1).start()

    weights.wait()

    def got_gated(i, c):
        gated_copy(i).wait()
        own_copy(i).wait()
        return c

    lax.fori_loop(0, half, got_gated, 0)

    def sent(d, c):
        state_copy(d).wait_send()
        decay_copy(d).wait_send()
        back_copy(d).wait_send()
        return c

    lax.fori_loop(1, n, sent, 0)
    state_done.wait()

def project(gown, gpeer, wown, wpeer, so, out, state):
    out[...] = (nn(gown[...], wown[...]) + nn(gpeer[...], wpeer[...])).astype(bf16)
    state[...] = so[...]


def per_device(
    queries, forget_logit, value_rows, out_gate, floor_gap, head_gain, state_in, out_weight
):
    n = lax.axis_size("sp")
    rows, width = queries.shape
    heads = state_in.shape[0]
    depth = out_weight.shape[1]
    blocks = rows // BLOCK
    kp = 128 // n
    tiles = depth // TILE
    mine = rows // 2
    V = pltpu.VMEM
    D = pltpu.SemaphoreType.DMA
    scratch = [
        V((rows, width), bf16), V((rows, width), bf16), V((rows, width), bf16), V((rows, width), bf16),
        V((1, width), f32), V((1, width), f32), V((heads, kp, 128), f32),
        V((rows, width), f32), V((rows, width), f32), V((blocks, heads, 128, 128), bf16),
        V((heads, 128, 128), f32), V((1, width), f32), V((blocks, 1, width), f32),
        V((rows, width), f32), V((rows, width), f32), V((rows, width), bf16),
        V((blocks, 2 * BLOCK, width), bf16), V((rows, width), bf16), V((rows, width), bf16),
        V((blocks, 1, width), f32), V((rows, width), bf16), V((mine, width), bf16),
        V((heads, kp * 128), f32),
        V((n, heads, kp, 128), bf16), V((heads, 128), f32), V((n, heads, kp, 128), bf16),
        V((n, heads, 128), f32), V((n * 8, 128), f32), V((128, n * 8), f32),
        V((n, heads, kp, 128), bf16), V((n, heads, kp, 128), bf16),
        V((mine, width), bf16),
        D((5,)), D((blocks,)), D((blocks,)), D((n,)), D((n,)), D((n,)), D((n,)), D((n,)), D((n,)),
        D((blocks // 2,)), D((blocks // 2,)), D((2,)), D((blocks // 2,)), D(()),
    ]
    gown, gpeer, wpeer, so = pl.pallas_call(
        functools.partial(kernel, (n, heads, blocks, kp)),
        name="layer",
        out_shape=(
            jax.ShapeDtypeStruct((mine, width), bf16),
            jax.ShapeDtypeStruct((mine, width), bf16),
            jax.ShapeDtypeStruct((width, depth), bf16),
            jax.ShapeDtypeStruct((heads, kp * 128), f32),
        ),
        in_specs=[pl.BlockSpec(memory_space=pltpu.HBM)] * 8,
        out_specs=(pl.BlockSpec(memory_space=pltpu.HBM),) * 4,
        scratch_shapes=scratch,
        compiler_params=pltpu.CompilerParams(
            collective_id=0, has_side_effects=True, vmem_limit_bytes=VMEM_LAYER
        ),
    )(
        forget_logit, value_rows, queries, out_gate,
        floor_gap.reshape(1, width), head_gain.reshape(1, width), state_in, out_weight,
    )
    whole = lambda t: (0, 0)
    piece = lambda t: (0, t)
    projected, state_out = pl.pallas_call(
        project,
        name="project",
        grid=(tiles,),
        out_shape=(
            jax.ShapeDtypeStruct((mine, depth), bf16),
            jax.ShapeDtypeStruct((heads, kp * 128), f32),
        ),
        in_specs=[
            pl.BlockSpec((mine, width), whole), pl.BlockSpec((mine, width), whole),
            pl.BlockSpec((width, TILE), piece), pl.BlockSpec((width, TILE), piece),
            pl.BlockSpec((heads, kp * 128), whole),
        ],
        out_specs=(pl.BlockSpec((mine, TILE), piece), pl.BlockSpec((heads, kp * 128), whole)),
        compiler_params=pltpu.CompilerParams(vmem_limit_bytes=VMEM_LAYER),
    )(gown, gpeer, out_weight, wpeer, so)
    return (projected, state_out)


def solution(mesh):
    placed = (
        P("sp", "tp"),
        P("sp", "tp"),
        P("sp", "tp"),
        P("sp", "tp"),
        P("tp"),
        P("tp"),
        P("tp", None, None),
        P("tp", None),
    )
    return jax.shard_map(
        per_device,
        mesh=mesh,
        in_specs=placed,
        out_specs=(P(("sp", "tp"), None), P("tp", "sp")),
        check_vma=False,
    )
```

```python
import functools

import jax
import jax.numpy as jnp
from jax import lax
from jax.experimental import pallas as pl
from jax.experimental.pallas import tpu as pltpu
from jax.sharding import PartitionSpec as P

BLOCK = 128
TILE = 512
epsilon = 1e-06
MESH = pl.DeviceIdType.MESH
f32 = jnp.float32
bf16 = jnp.bfloat16
VMEM_LAYER = 60 * 1024 * 1024
LOG_TERMS = (0.248358778, 0.245560933, 0.33349572, 0.49999794, 1.0)


def nt(a, b):
    return lax.dot_general(a, b, (((1,), (1,)), ((), ())), preferred_element_type=f32)


def tn(a, b):
    return lax.dot_general(a, b, (((0,), (0,)), ((), ())), preferred_element_type=f32)


def nn(a, b):
    return jnp.dot(a, b, preferred_element_type=f32)


def log_keep(g):
    series = LOG_TERMS[0]
    for term in LOG_TERMS[1:]:
        series = series * g + term
    return -g * series


def kernel(
    dims,
    fl_any, v_any, q_any, og_any, gap_any, gain_any, st_any, w_any,
    gown_out, gpeer, wpeer, so_out,
    fl, v, q, og, gap, gain, stin,
    cumul, kg, sbef, run, lt, es, raw, sg, qs2,
    hl, kst, dec, eb, qsc, gown, so,
    sbuf, dmine, rbuf, dbuf, dall, tcol, obuf, ibuf, gsend,
    in_sem, fl_sem, v_sem, s1, r1, sd, rd, s2, r2, gs, gr, wsem, gown_sem, so_sem,
):
    n, heads, blocks, kp = dims
    me = lax.axis_index("sp")
    core = lax.axis_index("tp")
    mate = 1 - core
    half = blocks // 2

    def local(i, src, dst):
        return pltpu.make_async_copy(src, dst, in_sem.at[i])

    def early(b):
        rows = pl.ds(pl.multiple_of(b * BLOCK, BLOCK), BLOCK)
        return (
            pltpu.make_async_copy(fl_any.at[rows], fl.at[rows], fl_sem.at[b]),
            pltpu.make_async_copy(v_any.at[rows], v.at[rows], v_sem.at[b]),
        )

    def start_early(b, c):
        for copy in early(b):
            copy.start()
        return c

    gap_load = local(0, gap_any, gap)
    gap_load.start()
    lax.fori_loop(0, blocks, start_early, 0)
    loads = [
        local(1, q_any, q), local(2, og_any, og), local(3, gain_any, gain),
        local(4, st_any.at[:, pl.ds(me * kp, kp), :], stin),
    ]

    barrier = pltpu.get_barrier_semaphore()

    def greet(d, c):
        pl.semaphore_signal(barrier, inc=1, device_id={"sp": lax.rem(me + d, n)}, device_id_type=MESH)
        return c

    lax.fori_loop(1, n, greet, 0)
    pl.semaphore_signal(barrier, inc=1, device_id={"tp": mate}, device_id_type=MESH)

    row = lax.broadcasted_iota(jnp.int32, (BLOCK, BLOCK), 0)
    col = lax.broadcasted_iota(jnp.int32, (BLOCK, BLOCK), 1)
    causal = row >= col
    lower = jnp.where(causal, 1.0, 0.0).astype(bf16)
    lower2 = jnp.concatenate([lower, lower], axis=1)

    run[...] = jnp.zeros_like(run)
    lt[...] = jnp.zeros_like(lt)
    dall[...] = jnp.zeros_like(dall)
    gap_load.wait()

    def block_rows(b):
        return pl.ds(pl.multiple_of(b * BLOCK, BLOCK), BLOCK)

    def gates(b, c):
        rows = block_rows(b)
        for copy in early(b):
            copy.wait()
        for h in range(heads):
            cols = slice(h * 128, (h + 1) * 128)
            x = fl[rows, cols].astype(f32)
            g = gap[:, cols] * (1.0 / (1.0 + jnp.exp(x)))
            lf = log_keep(g)
            hi = lf.astype(bf16)
            kg[rows, cols] = g
            hl[b, 0:BLOCK, cols] = hi
            hl[b, BLOCK:, cols] = (lf - hi.astype(f32)).astype(bf16)
        return c

    def sums(b, c):
        cumul[block_rows(b), :] = nn(lower2, hl[b])
        return c

    def decayed(b, c):
        rows = block_rows(b)
        es[b] = jnp.exp(lt[...])
        last = cumul[pl.ds(b * BLOCK + BLOCK - 1, 1), :]
        lt[...] = lt[...] + last
        keep = jnp.exp(last)
        eb[b] = keep
        for h in range(heads):
            cols = slice(h * 128, (h + 1) * 128)
            keys = kg[rows, cols] * jnp.exp(-cumul[rows, cols])
            kst[rows, cols] = keys.astype(bf16)
            dec[rows, cols] = (keys * keep[:, cols]).astype(bf16)
        return c

    def states(b, c):
        rows = block_rows(b)
        for h in range(heads):
            cols = slice(h * 128, (h + 1) * 128)
            old = run[h]
            sbef[b, h] = old.astype(bf16)
            run[h] = old * eb[b][:, cols] + tn(v[rows, cols], dec[rows, cols])
        return c

    with jax.named_scope("gates"):
        lax.fori_loop(0, blocks, gates, 0)
    with jax.named_scope("sums"):
        lax.fori_loop(0, blocks, sums, 0, unroll=4)
    with jax.named_scope("decayed"):
        lax.fori_loop(0, blocks, decayed, 0)
    with jax.named_scope("states"):
        lax.fori_loop(0, blocks, states, 0, unroll=4)
    for load in loads:
        load.start()

    for h in range(heads):
        cols = slice(h * 128, (h + 1) * 128)
        sbuf[:, h] = run[h].T.reshape(n, kp, 128).astype(bf16)
        dmine[h : h + 1, :] = jnp.exp(lt[:, cols])

    pl.semaphore_wait(barrier, n)

    def state_copy(d):
        to = lax.rem(me + d, n)
        return pltpu.make_async_remote_copy(
            src_ref=sbuf.at[to], dst_ref=rbuf.at[me], send_sem=s1.at[d], recv_sem=r1.at[d],
            device_id={"sp": to}, device_id_type=MESH)

    def decay_copy(d):
        return pltpu.make_async_remote_copy(
            src_ref=dmine, dst_ref=dbuf.at[me], send_sem=sd.at[d], recv_sem=rd.at[d],
            device_id={"sp": lax.rem(me + d, n)}, device_id_type=MESH)

    def back_copy(d):
        to = lax.rem(me + d, n)
        return pltpu.make_async_remote_copy(
            src_ref=obuf.at[to], dst_ref=ibuf.at[me], send_sem=s2.at[d], recv_sem=r2.at[d],
            device_id={"sp": to}, device_id_type=MESH)

    def send_states(d, c):
        state_copy(d).start()
        decay_copy(d).start()
        return c

    lax.fori_loop(1, n, send_states, 0)
    weights = pltpu.make_async_remote_copy(
        src_ref=w_any, dst_ref=wpeer, send_sem=wsem.at[0], recv_sem=wsem.at[1],
        device_id={"tp": mate}, device_id_type=MESH)
    weights.start()
    rbuf[me] = sbuf[me]
    dbuf[me] = dmine[...]

    for load in loads:
        load.wait()

    def reads(b, c):
        rows = block_rows(b)
        start = es[b]
        for h in range(heads):
            cols = slice(h * 128, (h + 1) * 128)
            hq = 0.5 * q[rows, cols].astype(f32)
            scaled = (hq + hq * jnp.tanh(hq)) * jnp.exp(cumul[rows, cols])
            qsc[rows, cols] = scaled.astype(bf16)
            qs2[rows, cols] = (scaled * start[:, cols]).astype(bf16)
            hg = 0.5 * og[rows, cols].astype(f32)
            sg[rows, cols] = (hg + hg * jnp.tanh(hg)) * gain[:, cols]
        return c

    def within(b, c):
        rows = block_rows(b)
        for h in range(heads):
            cols = slice(h * 128, (h + 1) * 128)
            qs = qsc[rows, cols]
            scores = jnp.where(causal, nt(qs, kst[rows, cols]), 0.0).astype(bf16)
            raw[rows, cols] = nn(scores, v[rows, cols]) + nt(qs, sbef[b, h])
        return c

    with jax.named_scope("reads"):
        lax.fori_loop(0, blocks, reads, 0)

    def got_states(d, c):
        state_copy(d).wait_recv()
        decay_copy(d).wait_recv()
        return c

    with jax.named_scope("wait1"):
        lax.fori_loop(1, n, got_states, 0)

    def spread(j, c):
        dall[pl.ds(j * 8, heads), :] = dbuf[j]
        return c

    lax.fori_loop(0, n, spread, 0)
    tcol[...] = dall[...].T
    decays = tcol[pl.ds(me * kp, kp), :]
    for h in range(heads):
        state = stin[h]
        for j in range(n):
            obuf[j, h] = state.astype(bf16)
            state = decays[:, 8 * j + h : 8 * j + h + 1] * state + rbuf[j, h].astype(f32)
        for k in range(kp):
            so[h : h + 1, k * 128 : (k + 1) * 128] = state[k : k + 1, :]
    ibuf[me] = obuf[me]

    def send_back(d, c):
        back_copy(d).start()
        return c

    lax.fori_loop(1, n, send_back, 0)
    state_done = pltpu.make_async_copy(so, so_out, so_sem)
    state_done.start()

    with jax.named_scope("within"):
        lax.fori_loop(0, blocks, within, 0, unroll=6)

    def got_back(d, c):
        back_copy(d).wait_recv()
        return c

    with jax.named_scope("wait2"):
        lax.fori_loop(1, n, got_back, 0)
    incoming = [ibuf[:, h].astype(f32).reshape(n * kp, 128).astype(bf16) for h in range(heads)]

    def finish(rows, h):
        cols = slice(h * 128, (h + 1) * 128)
        out = raw[rows, cols] + nn(qs2[rows, cols], incoming[h])
        mean = jnp.mean(out * out, axis=-1, keepdims=True)
        return (out * lax.rsqrt(mean + epsilon) * sg[rows, cols]).astype(bf16)

    def gated_copy(i):
        rows = pl.ds(pl.multiple_of(i * BLOCK, BLOCK), BLOCK)
        return pltpu.make_async_remote_copy(
            src_ref=gsend.at[rows], dst_ref=gpeer.at[rows], send_sem=gs.at[i], recv_sem=gr.at[i],
            device_id={"tp": mate}, device_id_type=MESH)

    def theirs(i, c):
        rows = pl.ds(pl.multiple_of((mate * half + i) * BLOCK, BLOCK), BLOCK)
        to = pl.ds(pl.multiple_of(i * BLOCK, BLOCK), BLOCK)
        for h in range(heads):
            gsend[to, h * 128 : (h + 1) * 128] = finish(rows, h)

        @pl.when(i > 0)
        def _():
            gated_copy(i - 1).start()

        return c

    with jax.named_scope("theirs"):
        lax.fori_loop(0, half, theirs, 0, unroll=3)
    gated_copy(half - 1).start()

    def mine(i, c):
        rows = pl.ds(pl.multiple_of((core * half + i) * BLOCK, BLOCK), BLOCK)
        to = pl.ds(pl.multiple_of(i * BLOCK, BLOCK), BLOCK)
        for h in range(heads):
            gown[to, h * 128 : (h + 1) * 128] = finish(rows, h)

        @pl.when(i > 0)
        def _():
            own_copy(i - 1).start()

        return c

    def own_copy(i):
        rows = block_rows(i)
        return pltpu.make_async_copy(gown.at[rows], gown_out.at[rows], gown_sem.at[i])

    with jax.named_scope("mine"):
        lax.fori_loop(0, half, mine, 0, unroll=3)
    own_copy(half - 1).start()

    weights.wait()

    def got_gated(i, c):
        gated_copy(i).wait()
        own_copy(i).wait()
        return c

    lax.fori_loop(0, half, got_gated, 0)

    def sent(d, c):
        state_copy(d).wait_send()
        decay_copy(d).wait_send()
        back_copy(d).wait_send()
        return c

    lax.fori_loop(1, n, sent, 0)
    state_done.wait()

def project(gown, gpeer, wown, wpeer, so, out, state):
    out[...] = (nn(gown[...], wown[...]) + nn(gpeer[...], wpeer[...])).astype(bf16)
    state[...] = so[...]


def per_device(
    queries, forget_logit, value_rows, out_gate, floor_gap, head_gain, state_in, out_weight
):
    n = lax.axis_size("sp")
    rows, width = queries.shape
    heads = state_in.shape[0]
    depth = out_weight.shape[1]
    blocks = rows // BLOCK
    kp = 128 // n
    tiles = depth // TILE
    mine = rows // 2
    V = pltpu.VMEM
    D = pltpu.SemaphoreType.DMA
    scratch = [
        V((rows, width), bf16), V((rows, width), bf16), V((rows, width), bf16), V((rows, width), bf16),
        V((1, width), f32), V((1, width), f32), V((heads, kp, 128), f32),
        V((rows, width), f32), V((rows, width), f32), V((blocks, heads, 128, 128), bf16),
        V((heads, 128, 128), f32), V((1, width), f32), V((blocks, 1, width), f32),
        V((rows, width), f32), V((rows, width), f32), V((rows, width), bf16),
        V((blocks, 2 * BLOCK, width), bf16), V((rows, width), bf16), V((rows, width), bf16),
        V((blocks, 1, width), f32), V((rows, width), bf16), V((mine, width), bf16),
        V((heads, kp * 128), f32),
        V((n, heads, kp, 128), bf16), V((heads, 128), f32), V((n, heads, kp, 128), bf16),
        V((n, heads, 128), f32), V((n * 8, 128), f32), V((128, n * 8), f32),
        V((n, heads, kp, 128), bf16), V((n, heads, kp, 128), bf16),
        V((mine, width), bf16),
        D((5,)), D((blocks,)), D((blocks,)), D((n,)), D((n,)), D((n,)), D((n,)), D((n,)), D((n,)),
        D((blocks // 2,)), D((blocks // 2,)), D((2,)), D((blocks // 2,)), D(()),
    ]
    gown, gpeer, wpeer, so = pl.pallas_call(
        functools.partial(kernel, (n, heads, blocks, kp)),
        name="layer",
        out_shape=(
            jax.ShapeDtypeStruct((mine, width), bf16),
            jax.ShapeDtypeStruct((mine, width), bf16),
            jax.ShapeDtypeStruct((width, depth), bf16),
            jax.ShapeDtypeStruct((heads, kp * 128), f32),
        ),
        in_specs=[pl.BlockSpec(memory_space=pltpu.HBM)] * 8,
        out_specs=(pl.BlockSpec(memory_space=pltpu.HBM),) * 4,
        scratch_shapes=scratch,
        compiler_params=pltpu.CompilerParams(
            collective_id=0, has_side_effects=True, vmem_limit_bytes=VMEM_LAYER
        ),
    )(
        forget_logit, value_rows, queries, out_gate,
        floor_gap.reshape(1, width), head_gain.reshape(1, width), state_in, out_weight,
    )
    whole = lambda t: (0, 0)
    piece = lambda t: (0, t)
    projected, state_out = pl.pallas_call(
        project,
        name="project",
        grid=(tiles,),
        out_shape=(
            jax.ShapeDtypeStruct((mine, depth), bf16),
            jax.ShapeDtypeStruct((heads, kp * 128), f32),
        ),
        in_specs=[
            pl.BlockSpec((mine, width), whole), pl.BlockSpec((mine, width), whole),
            pl.BlockSpec((width, TILE), piece), pl.BlockSpec((width, TILE), piece),
            pl.BlockSpec((heads, kp * 128), whole),
        ],
        out_specs=(pl.BlockSpec((mine, TILE), piece), pl.BlockSpec((heads, kp * 128), whole)),
        compiler_params=pltpu.CompilerParams(vmem_limit_bytes=VMEM_LAYER),
    )(gown, gpeer, out_weight, wpeer, so)
    return (projected, state_out)


def solution(mesh):
    placed = (
        P("sp", "tp"),
        P("sp", "tp"),
        P("sp", "tp"),
        P("sp", "tp"),
        P("tp"),
        P("tp"),
        P("tp", None, None),
        P("tp", None),
    )
    return jax.shard_map(
        per_device,
        mesh=mesh,
        in_specs=placed,
        out_specs=(P(("sp", "tp"), None), P("tp", "sp")),
        check_vma=False,
    )
```
